128 devices in a mesh: sp: 32 (over z, y, core), tp: 4 (over x).
Axes of the slice: x: 4, y: 4, z: 4, core: 2. Of those that a mesh axis runs over, the one named last changes fastest.
Arguments:
- residual: bfloat16 [32768, 2048], P('sp'), may hold values from -8 to 8
- query_wide: bfloat16 [32768, 1024], P('sp', 'tp'), may hold values from -6 to 6
- key_wide: bfloat16 [32768, 1024], P('sp', 'tp'), may hold values from -6 to 6
- value_wide: bfloat16 [32768, 2048], P('sp', 'tp'), may hold values from -6 to 6
- decay_wide: bfloat16 [32768, 1024], P('sp', 'tp'), may hold values from -12 to 12
- gate_wide: bfloat16 [32768, 2048], P('sp', 'tp'), may hold values from -6 to 6
- query_narrow: bfloat16 [32768, 512], P('sp', 'tp'), may hold values from -6 to 6
- key_narrow: bfloat16 [32768, 512], P('sp', 'tp'), may hold values from -6 to 6
- value_narrow: bfloat16 [32768, 2048], P('sp', 'tp'), may hold values from -6 to 6
- decay_narrow: bfloat16 [32768, 512], P('sp', 'tp'), may hold values from -12 to 12
- gate_narrow: bfloat16 [32768, 2048], P('sp', 'tp'), may hold values from -6 to 6
- head_gain: float32 [512], replicated, may hold values from 0.1 to 1.9
- out_wide: bfloat16 [2048, 2048], P('tp'), may hold values from -0.125 to 0.125
- out_narrow: bfloat16 [2048, 2048], P('tp'), may hold values from -0.125 to 0.125
- mlp_gain: float32 [2048], replicated, may hold values from 0.1 to 1.9
- up_weight: bfloat16 [2048, 4096], P('sp', 'tp'), may hold values from -0.125 to 0.125
- down_weight: bfloat16 [4096, 2048], P('tp', 'sp'), may hold values from -0.09375 to 0.09375
Outputs:
- layer_out: bfloat16 [32768, 2048], P('sp', 'tp')
The draws below stay inside these ranges and needn't reach their ends.
All inputs are finite; a program needn't handle non-finite values.
Results may differ from the reference program's by a relative error of at most 0.017.
Values may be sent and summed in bfloat16 or wider, within the bound.
A program may use at most 128 MiB of HBM per device.

```python
import math
import jax
import jax.numpy as jnp
from jax import lax

D = 2048
FF = 4096
HEADS = 4
HEAD_KA = 256
HEAD_KB = 128
HEAD_V = 512
BLOCK = 64
TOK_DEV = 1024
SEQUENCE_TOKENS = 32768
N_TP = 4


def draw_residual(key, part):
    column = jnp.arange(D, dtype=jnp.float32) / D
    baseline = jax.random.normal(jax.random.fold_in(key, 3), (SEQUENCE_TOKENS, D), jnp.float32)
    scale = 0.5 * jnp.power(4.0, column)
    return jnp.clip(baseline * scale[None, :], -8.0, 8.0).astype(jnp.bfloat16)


def decay_draw(key, head_width, salt):
    random_subkeys = jax.random.split(jax.random.fold_in(key, salt), 6)
    channel_count = HEADS * head_width
    ranking = jax.random.permutation(random_subkeys[0], HEADS)
    slow_heads = ranking < HEADS // 2
    jitter = jnp.clip(jax.random.normal(random_subkeys[1], (SEQUENCE_TOKENS, channel_count), jnp.float32), -3.0, 3.0)
    offsets = jax.random.uniform(random_subkeys[2], (SEQUENCE_TOKENS // TOK_DEV,), jnp.float32, -0.7, 0.7)
    slow_cols = jnp.repeat(slow_heads, head_width, total_repeat_length=channel_count)
    baseline = jnp.where(slow_cols, math.log(SEQUENCE_TOKENS / 4.0), 1.0)
    spread = jax.random.uniform(random_subkeys[3], (channel_count,), jnp.float32, -0.5, 0.5)
    grouped_rows = jax.random.randint(random_subkeys[4], (3,), 0, SEQUENCE_TOKENS)
    group_match = jnp.any(jnp.arange(SEQUENCE_TOKENS)[:, None] == grouped_rows[None, :], axis=1)
    group_depth = jax.random.uniform(random_subkeys[5], (SEQUENCE_TOKENS, 1), jnp.float32, 3.5, 8.0)
    row_offsets = jnp.repeat(offsets, TOK_DEV, total_repeat_length=SEQUENCE_TOKENS)
    before_activation = baseline[None, :] + spread[None, :] + row_offsets[:, None] + jitter
    before_activation = jnp.where(group_match[:, None], -group_depth, before_activation)
    return jnp.clip(before_activation, -12.0, 12.0).astype(jnp.bfloat16)


def draw_decay_wide(key, part):
    return decay_draw(key, HEAD_KA, 11)


def draw_decay_narrow(key, part):
    return decay_draw(key, HEAD_KB, 13)


def levels(rng, extent, pieces, least, largest):
    def one(dim, blocks):
        draws = jax.random.uniform(jax.random.fold_in(jax.random.fold_in(rng, 6), dim), (blocks,), jnp.float32, least / len(pieces), largest / len(pieces))
        return jnp.repeat(jnp.exp(draws), extent[dim] // blocks).reshape((-1,) + (1,) * (len(extent) - dim - 1))

    factor_of = one(*pieces[0])
    for cut in pieces[1:]:
        factor_of = factor_of * one(*cut)
    return factor_of


def centred(own_key, extent, scale, bound, pieces=(), kind=jnp.bfloat16):
    gain = levels(own_key, extent, pieces, -0.22, 0.18) if pieces else 1.0
    drawn = jax.random.normal(own_key, extent, jnp.float32) * scale * gain
    return jnp.minimum(jnp.maximum(drawn, -bound), bound).astype(kind)


def setup_inputs(seed: int = 0) -> dict:
    streams_of = jax.random.split(jax.random.key(seed), 18)
    residual = draw_residual(jax.random.fold_in(streams_of[17], 71), 0)
    query_wide = centred(streams_of[1], (SEQUENCE_TOKENS, HEADS * HEAD_KA), 1.0, 6.0, ((0, 32), (1, 4)))
    key_wide = centred(streams_of[2], (SEQUENCE_TOKENS, HEADS * HEAD_KA), 1.0, 6.0, ((0, 32), (1, 4)))
    value_wide = centred(streams_of[3], (SEQUENCE_TOKENS, HEADS * HEAD_V), 1.0, 6.0, ((0, 32), (1, 4)))
    decay_wide = draw_decay_wide(jax.random.fold_in(streams_of[17], 71), 0)
    gate_wide = centred(streams_of[5], (SEQUENCE_TOKENS, HEADS * HEAD_V), 1.0, 6.0, ((0, 32), (1, 4)))
    query_narrow = centred(streams_of[6], (SEQUENCE_TOKENS, HEADS * HEAD_KB), 1.0, 6.0, ((0, 32), (1, 4)))
    key_narrow = centred(streams_of[7], (SEQUENCE_TOKENS, HEADS * HEAD_KB), 1.0, 6.0, ((0, 32), (1, 4)))
    value_narrow = centred(streams_of[8], (SEQUENCE_TOKENS, HEADS * HEAD_V), 1.0, 6.0, ((0, 32), (1, 4)))
    decay_narrow = draw_decay_narrow(jax.random.fold_in(streams_of[17], 71), 0)
    gate_narrow = centred(streams_of[10], (SEQUENCE_TOKENS, HEADS * HEAD_V), 1.0, 6.0, ((0, 32), (1, 4)))
    head_gain = jnp.clip(1.0 + 0.18 * jax.random.normal(streams_of[11], (HEAD_V,), jnp.float32), 0.1, 1.9)
    out_wide = centred(streams_of[12], (HEADS * HEAD_V, D), (HEADS * HEAD_V) ** -0.5, 0.125, ((0, 4),))
    out_narrow = centred(streams_of[13], (HEADS * HEAD_V, D), (HEADS * HEAD_V) ** -0.5, 0.125, ((0, 4),))
    mlp_gain = jnp.clip(1.0 + 0.18 * jax.random.normal(streams_of[14], (D,), jnp.float32), 0.1, 1.9)
    up_weight = centred(streams_of[15], (D, FF), D ** -0.5, 0.125, ((0, 32), (1, 4)))
    down_weight = centred(streams_of[16], (FF, D), FF ** -0.5, 0.09375, ((0, 4), (1, 32)))
    return dict(residual=residual, query_wide=query_wide, key_wide=key_wide, value_wide=value_wide, decay_wide=decay_wide, gate_wide=gate_wide, query_narrow=query_narrow, key_narrow=key_narrow, value_narrow=value_narrow, decay_narrow=decay_narrow, gate_narrow=gate_narrow, head_gain=head_gain, out_wide=out_wide, out_narrow=out_narrow, mlp_gain=mlp_gain, up_weight=up_weight, down_weight=down_weight)


EPS = 1e-05
DECAY_NORMALIZER = 16.0
HIGHEST = lax.Precision.HIGHEST

def block_pass(queries, keys_in, values_in, log_decay, block_len):
    num_blocks = queries.shape[0] // block_len

    def to_blocks(stacked):
        return stacked.reshape((num_blocks, block_len) + stacked.shape[1:])
    causal = jnp.tril(jnp.ones((block_len, block_len), dtype=bool))
    initial = (jnp.zeros((queries.shape[1], queries.shape[2], values_in.shape[2]), jnp.float32), jnp.zeros((queries.shape[1], queries.shape[2]), jnp.float32))

    def advance(running, inputs):
        memory, offset = running
        block_q, block_k, block_v, block_g = inputs
        within = jnp.cumsum(block_g, axis=0)
        final_log = within[-1]
        scaled_q = block_q * jnp.exp(within)
        scaled_k = block_k * jnp.exp(-within)
        outside = jnp.einsum('ihd,hde->ihe', scaled_q, memory, precision=HIGHEST)
        scores = jnp.einsum('ihd,jhd->hij', scaled_q, scaled_k, precision=HIGHEST)
        scores = jnp.where(causal[None], scores, 0.0)
        inside = jnp.einsum('hij,jhe->ihe', scores, block_v, precision=HIGHEST)
        decayed_keys = scaled_k * jnp.exp(final_log)[None]
        memory = jnp.exp(final_log)[..., None] * memory + jnp.einsum('jhd,jhe->hde', decayed_keys, block_v, precision=HIGHEST)
        carried_q = scaled_q * jnp.exp(offset)[None]
        return ((memory, offset + final_log), (outside + inside, carried_q))
    (memory, totals), (outputs, carried_q) = lax.scan(advance, initial, (to_blocks(queries), to_blocks(keys_in), to_blocks(values_in), to_blocks(log_decay)))
    return (outputs.reshape(values_in.shape), carried_q.reshape(queries.shape), totals, memory)

def prepare(query, key_proj, value, decay, heads_here):
    row_count = query.shape[0]
    key_width = query.shape[1] // heads_here
    queries = query.astype(jnp.float32).reshape(row_count, heads_here, key_width) * key_width ** (-0.5)
    keys_in = key_proj.astype(jnp.float32).reshape(row_count, heads_here, key_width)
    values_in = value.astype(jnp.float32).reshape(row_count, heads_here, value.shape[1] // heads_here)
    log_decay = jax.nn.log_sigmoid(decay.astype(jnp.float32)).reshape(row_count, heads_here, key_width) / DECAY_NORMALIZER
    return (queries, keys_in, values_in, log_decay)

def finish(outputs, gate, head_gain):
    scale = lax.rsqrt(lax.optimization_barrier(jnp.mean(jnp.square(outputs), axis=-1, keepdims=True)) + EPS)
    gated = outputs * scale * head_gain * jax.nn.silu(gate.astype(jnp.float32).reshape(outputs.shape))
    return gated.reshape(outputs.shape[0], -1).astype(jnp.bfloat16)

def group_output(query, key_proj, value, decay, gate, head_gain):
    queries, keys_in, values_in, log_decay = prepare(query, key_proj, value, decay, HEADS)
    outputs = block_pass(queries, keys_in, values_in, log_decay, BLOCK)[0]
    return finish(outputs, gate, head_gain)

def blockwise_sum(left_sides, right_sides):
    total = jnp.zeros((left_sides[0].shape[0], right_sides[0].shape[1]), jnp.float32)
    for tp_block in range(N_TP):
        block_sum = jnp.zeros_like(total)
        for left_side, right_side in zip(left_sides, right_sides):
            block_width = left_side.shape[1] // N_TP
            first_col = tp_block * block_width
            block_sum = block_sum + jnp.dot(left_side[:, first_col:first_col + block_width], right_side[first_col:first_col + block_width], preferred_element_type=jnp.float32)
        total = total + lax.optimization_barrier(block_sum.astype(jnp.bfloat16)).astype(jnp.float32)
    return total

def reference(residual, query_wide, key_wide, value_wide, decay_wide, gate_wide, query_narrow, key_narrow, value_narrow, decay_narrow, gate_narrow, head_gain, out_wide, out_narrow, mlp_gain, up_weight, down_weight):
    gated_wide = group_output(query_wide, key_wide, value_wide, decay_wide, gate_wide, head_gain)
    gated_narrow = group_output(query_narrow, key_narrow, value_narrow, decay_narrow, gate_narrow, head_gain)
    mixed = blockwise_sum((gated_wide, gated_narrow), (out_wide, out_narrow))
    stream = (residual.astype(jnp.float32) + mixed).astype(jnp.bfloat16)
    stream_f = stream.astype(jnp.float32)
    normed = (stream_f * lax.rsqrt(lax.optimization_barrier(jnp.mean(jnp.square(stream_f), axis=1, keepdims=True)) + EPS) * mlp_gain).astype(jnp.bfloat16)
    hidden = jnp.square(jax.nn.relu(jnp.dot(normed, up_weight, preferred_element_type=jnp.float32))).astype(jnp.bfloat16)
    mlp_sum = blockwise_sum((hidden,), (down_weight,))
    return (stream_f + mlp_sum).astype(jnp.bfloat16)
```

```python
import jax
import jax.numpy as jnp
from jax import lax
from jax.experimental import pallas as pl
from jax.experimental.pallas import tpu as pltpu
from jax.sharding import PartitionSpec as P

MESH = pl.DeviceIdType.MESH
F32, BF16 = jnp.float32, jnp.bfloat16
EPS = 1e-05
C = 128
CH = 8
KA, KB, KK = 256, 128, 384
S = 4
R = 64
D = 2048
H = 1024


def dot(a, b):
    return jnp.dot(a, b, preferred_element_type=F32)


def dot_nt(a, b):
    return lax.dot_general(a, b, (((1,), (1,)), ((), ())), preferred_element_type=F32)


def dot_tn(a, b):
    return lax.dot_general(a, b, (((0,), (0,)), ((), ())), preferred_element_type=F32)


def kernel(
    res, qw, kw, vw, dw, gw, qn, kn, vn, dn, gn, ow, on, upw, dnw, gain, mgain,
    out,
    q_s, k_s, d_s, v_s, g_s, o_s, res_s, xw, up, down, qd, qo, mc, m_s, sb, dt,
    r1, rd1, t2, dt2, r2, rd2, s3, m_in, att, px, rxa, rxb, st, xs, py, rya, ryb, hid, fin, outb,
    ld, w1s, w1r, w2s, w2r, w3s, w3r, w3fs, w3fr, w4s, w4r,
    s1s, s1r, s1ds, s1dr, s2s, s2r, s2ds, s2dr, s3s, s3r,
    xas, xar, xbs, xbr, yas, yar, ybs, ybr, ags, agr, afs, afr, oas, oar, ods,
):
    sp = lax.axis_index("sp")
    x = lax.axis_index("tp")
    core = lax.rem(sp, 2)
    y = lax.rem(lax.div(sp, 2), 4)
    z = lax.div(sp, 8)
    me = lax.rem(sp, 8)

    def at(xx, yy, zz, cc):
        return ((zz * 4 + yy) * 2 + cc, xx)

    def m4(v):
        return lax.rem(v + 8, 4)

    def remote(src, dst, ss, rs, dev):
        return pltpu.make_async_remote_copy(
            src_ref=src, dst_ref=dst, send_sem=ss, recv_sem=rs, device_id=dev, device_id_type=MESH
        )

    tok = pl.ds(pl.multiple_of(x * (S * R), S * R), S * R)
    loads = [
        (upw, xw.at[x, 0:64]),
        (dnw, xw.at[x, 64:128]),
        (dw, d_s.at[:, 0:KA]),
        (dn, d_s.at[:, KA:KK]),
        (kw, k_s.at[:, 0:KA]),
        (kn, k_s.at[:, KA:KK]),
        (qw, q_s.at[:, 0:KA]),
        (qn, q_s.at[:, KA:KK]),
        (vw, v_s.at[:, 0:512]),
        (vn, v_s.at[:, 512:1024]),
        (gw, g_s.at[:, 0:512]),
        (gn, g_s.at[:, 512:1024]),
        (ow, o_s.at[0:512]),
        (on, o_s.at[512:1024]),
        (res.at[tok], res_s),
    ]
    loads = [pltpu.make_async_copy(a, b, ld.at[i]) for i, (a, b) in enumerate(loads)]
    for c in loads:
        c.start()

    barrier = pltpu.get_barrier_semaphore()
    for d in (1, 2, 3):
        pl.semaphore_signal(barrier, inc=1, device_id=at(m4(x + d), y, z, core), device_id_type=MESH)
        pl.semaphore_signal(barrier, inc=1, device_id=at(x, y, m4(z + d), core), device_id_type=MESH)
    for d in range(1, 8):
        j = lax.rem(me + d, 8)
        pl.semaphore_signal(barrier, inc=1, device_id=(z * 8 + j, x), device_id_type=MESH)
    pl.semaphore_wait(barrier, 13)

    def w1(d):
        t = m4(x + d)
        return remote(xw.at[x], xw.at[x], w1s.at[t], w1r.at[x], at(t, y, z, core))

    loads[0].wait()
    loads[1].wait()
    for d in (1, 3, 2):
        w1(d).start()

    row_i = lax.broadcasted_iota(jnp.int32, (C, C), 0)
    col_i = lax.broadcasted_iota(jnp.int32, (C, C), 1)
    causal = col_i <= row_i
    lower = causal.astype(BF16)
    lane = lax.broadcasted_iota(jnp.int32, (1, KK), 1)
    scale = jnp.where(lane < KA, KA**-0.5, KB**-0.5).astype(F32)
    for c in loads[2:10]:
        c.wait()
    m_s[...] = jnp.zeros_like(m_s)

    def first(c, off):
        rows = pl.ds(pl.multiple_of(c * C, C), C)
        dd = d_s[rows, :].astype(F32)
        g = (jnp.minimum(dd, 0.0) - jnp.log1p(jnp.exp(-jnp.abs(dd)))) * (1.0 / 16.0)
        high = g.astype(BF16)
        low = (g - high.astype(F32)).astype(BF16)
        within = dot(lower, high) + dot(lower, low)
        mid = within[C // 2 - 1 : C // 2, :]
        last = within[C - 1 : C, :]
        qf = q_s[rows, :].astype(F32) * scale
        kf = k_s[rows, :].astype(F32)
        decayed = qf * jnp.exp(within)
        q_s[rows, :] = (qf * jnp.exp(within - mid)).astype(BF16)
        k_s[rows, :] = (kf * jnp.exp(mid - within)).astype(BF16)
        qd[rows, :] = decayed.astype(BF16)
        qo[rows, :] = (decayed * jnp.exp(off)).astype(BF16)
        kd = (kf * jnp.exp(last - within)).astype(BF16)
        mc[c] = m_s[...].astype(BF16)
        fade = jnp.exp(last)
        m_s[:, 0:KA] = m_s[:, 0:KA] * fade[:, 0:KA] + dot_tn(v_s[rows, 0:512], kd[:, 0:KA])
        m_s[:, KA:KK] = m_s[:, KA:KK] * fade[:, KA:KK] + dot_tn(v_s[rows, 512:1024], kd[:, KA:KK])
        return off + last

    total = lax.fori_loop(0, CH, first, jnp.zeros((1, KK), F32))
    sb[...] = m_s[...].astype(BF16)
    dt[...] = jnp.broadcast_to(total, (8, KK))

    def part(j):
        return pl.ds(pl.multiple_of(j * 64, 64), 64)

    def s1(d):
        j = lax.rem(me + d, 8)
        dev = (z * 8 + j, x)
        return (
            remote(sb.at[part(j)], r1.at[me], s1s.at[j], s1r.at[me], dev),
            remote(dt, rd1.at[me], s1ds.at[j], s1dr.at[me], dev),
        )

    for d in range(1, 8):
        for c in s1(d):
            c.start()
    r1[me] = sb[part(me), :]
    rd1[me] = dt[...]

    own = pl.ds(pl.multiple_of(sp * 64, 64), 64)

    def w2(d):
        q = m4(x + y + d)
        dev = at(x, m4(y + d), z, core)
        return (
            remote(xw.at[q, 0:64], up.at[own], w2s.at[0, q], w2r.at[0, y], dev),
            remote(xw.at[q, 64:128], down.at[own], w2s.at[1, q], w2r.at[1, y], dev),
        )

    def second(c, _):
        rows = pl.ds(pl.multiple_of(c * C, C), C)
        for ks, vs in ((slice(0, KA), slice(0, 512)), (slice(KA, KK), slice(512, 1024))):
            sc = dot_nt(q_s[rows, ks], k_s[rows, ks])
            sc = jnp.where(causal, sc, 0.0).astype(BF16)
            att[rows, vs] = dot(sc, v_s[rows, vs]) + dot_nt(qd[rows, ks], mc[c, :, ks])
        return 0

    lax.fori_loop(0, CH, second, 0)

    for d in range(1, 8):
        j = lax.rem(me + d, 8)
        remote(sb.at[part(me)], r1.at[j], s1s.at[j], s1r.at[j], (z * 8 + j, x)).wait_recv()
        remote(dt, rd1.at[j], s1ds.at[j], s1dr.at[j], (z * 8 + j, x)).wait_recv()

    def over_cores(j, carry):
        acc, dacc = carry
        dj = rd1[j][0:1, :]
        return acc * jnp.exp(dj) + r1[j].astype(F32), dacc + dj

    acc, dacc = lax.fori_loop(
        0, 8, over_cores, (jnp.zeros((64, KK), F32), jnp.zeros((1, KK), F32))
    )
    t2[...] = acc.astype(BF16)
    dt2[...] = jnp.broadcast_to(dacc, (8, KK))

    def s2(d):
        t = m4(z + d)
        dev = at(x, y, t, core)
        return (
            remote(t2, r2.at[z], s2s.at[t], s2r.at[z], dev),
            remote(dt2, rd2.at[z], s2ds.at[t], s2dr.at[z], dev),
        )

    for d in (1, 3, 2):
        for c in s2(d):
            c.start()
    r2[z] = t2[...]
    rd2[z] = dt2[...]
    for d in (1, 2, 3):
        t = m4(x + d)
        remote(xw.at[t], xw.at[t], w1s.at[t], w1r.at[t], at(t, y, z, core)).wait_recv()
    quarter = m4(x + y)
    up[own, :] = xw[quarter, 0:64]
    down[own, :] = xw[quarter, 64:128]
    for d in (1, 2, 3):
        t = m4(z + d)
        remote(t2, r2.at[t], s2s.at[t], s2r.at[t], at(x, y, t, core)).wait_recv()
        remote(dt2, rd2.at[t], s2ds.at[t], s2dr.at[t], at(x, y, t, core)).wait_recv()

    def over_z(t, acc):
        return jnp.where(t < z, acc * jnp.exp(rd2[t][0:1, :]) + r2[t].astype(F32), acc)

    acc = lax.fori_loop(0, 4, over_z, jnp.zeros((64, KK), F32))

    def hand_out(j, acc):
        s3[j] = acc.astype(BF16)
        return acc * jnp.exp(rd1[j][0:1, :]) + r1[j].astype(F32)

    lax.fori_loop(0, 8, hand_out, acc)

    def s3c(d):
        j = lax.rem(me + d, 8)
        return remote(s3.at[j], m_in.at[part(me)], s3s.at[j], s3r.at[me], (z * 8 + j, x))

    for d in range(1, 8):
        s3c(d).start()
    m_in[part(me), :] = s3[me]

    for d in (1, 3, 2):
        for c in w2(d):
            c.start()

    def piece(zz, p):
        return pl.ds(pl.multiple_of(((zz * 4 + p) * 2 + core) * 64, 64), 64)

    def w3(p, kind, side):
        ref = (up, down)[kind]
        rows = piece(z, p)
        dev = at(x, y, m4(z + (1, -1)[side]), core)
        return remote(ref.at[rows], ref.at[rows], w3s.at[side, kind, p], w3r.at[side, kind, p], dev)

    def w3_got(p, kind, side):
        ref = (up, down)[kind]
        rows = piece(m4(z - (1, -1)[side]), p)
        dev = at(x, y, m4(z - (1, -1)[side]), core)
        return remote(ref.at[rows], ref.at[rows], w3s.at[side, kind, p], w3r.at[side, kind, p], dev)

    def w3f(p, side):
        ref = (up, down)[side]
        rows = piece(m4(z - (1, -1)[side]), p)
        dev = at(x, y, m4(z + (1, -1)[side]), core)
        return remote(ref.at[rows], ref.at[rows], w3fs.at[side, p], w3fr.at[side, p], dev)

    def w3f_got(p, side):
        ref = (up, down)[side]
        rows = piece(m4(z + 2), p)
        dev = at(x, y, m4(z - (1, -1)[side]), core)
        return remote(ref.at[rows], ref.at[rows], w3fs.at[side, p], w3fr.at[side, p], dev)

    def w4(zz, p, kind):
        ref = (up, down)[kind]
        rows = piece(zz, p)
        dev = at(x, y, z, 1 - core)
        return remote(ref.at[rows], ref.at[rows], w4s.at[kind, zz, p], w4r.at[kind, zz, p], dev)

    def w4_got(zz, p, kind):
        ref = (up, down)[kind]
        rows = pl.ds(pl.multiple_of(((zz * 4 + p) * 2 + 1 - core) * 64, 64), 64)
        dev = at(x, y, z, 1 - core)
        return remote(ref.at[rows], ref.at[rows], w4s.at[kind, zz, p], w4r.at[kind, zz, p], dev)

    for d in range(1, 8):
        j = lax.rem(me + d, 8)
        remote(s3.at[j], m_in.at[part(j)], s3s.at[j], s3r.at[j], (z * 8 + j, x)).wait_recv()

    def own_pieces(d):
        p = m4(y + d)
        if d:
            for kind in (0, 1):
                ref = (up, down)[kind]
                rows = piece(z, p)
                remote(
                    ref.at[rows], ref.at[rows], w2s.at[kind, p], w2r.at[kind, p], at(x, p, z, core)
                ).wait_recv()
        for kind, side in ((0, 0), (1, 1), (1, 0), (0, 1)):
            w3(p, kind, side).start()
        for kind in (0, 1):
            w4(z, p, kind).start()

    def near_pieces(p):
        for kind in (0, 1):
            w3_got(p, kind, kind).wait_recv()
            w3f(p, kind).start()
        for kind in (0, 1):
            w3_got(p, kind, 1 - kind).wait_recv()
        for kind in (0, 1):
            w4(m4(z + 1), p, kind).start()
            w4(m4(z - 1), p, kind).start()

    def far_pieces(p):
        for kind in (0, 1):
            w3f_got(p, kind).wait_recv()
        for kind in (0, 1):
            w4(m4(z + 2), p, kind).start()

    for c in loads[10:]:
        c.wait()

    low, high = slice(0, H), slice(H, D)

    class Ring:
        def __init__(self, coord, dev, p, ra, rb, a_s, a_r, b_s, b_r):
            self.c, self.dev, self.p, self.ra, self.rb = coord, dev, p, ra, rb
            self.a_s, self.a_r, self.b_s, self.b_r = a_s, a_r, b_s, b_r

        def up_of(self, k):
            return m4(self.c + k)

        def relay(self, s, side):
            far = self.p.at[s, self.up_of(2), :, (high, low)[side]]
            dev = self.dev(self.up_of((1, -1)[side]))
            return remote(far, self.ra.at[s, side], self.a_s.at[s, side], self.a_r.at[s, side], dev)

        def near(self, s, side, half):
            t = self.up_of((1, -1)[side])
            cols = (low, high)[half]
            return remote(
                self.p.at[s, t, :, cols], self.rb.at[s, side, :, cols],
                self.b_s.at[s, side, half], self.b_r.at[s, side, half], self.dev(t),
            )

        def begin(self, s):
            for side in (0, 1):
                self.relay(s, side).start()
            for side in (0, 1):
                self.near(s, side, side).start()

        def middle(self, s):
            for side in (0, 1):
                self.relay(s, side).wait_recv()
                t = self.up_of((1, -1)[side])
                cols = (high, low)[side]
                self.p[s, t, :, cols] = (
                    self.p[s, t, :, cols].astype(F32) + self.ra[s, side].astype(F32)
                ).astype(BF16)
                self.near(s, side, 1 - side).start()

        def end(self, s):
            for side in (0, 1):
                for half in (0, 1):
                    self.near(s, side, half).wait_recv()
            return (
                self.p[s, self.c].astype(F32)
                + self.rb[s, 0].astype(F32)
                + self.rb[s, 1].astype(F32)
            )

        def drain(self, s):
            for side in (0, 1):
                self.relay(s, side).wait_send()
                for half in (0, 1):
                    self.near(s, side, half).wait_send()

    ring_x = Ring(x, lambda t: at(t, y, z, core), px, rxa, rxb, xas, xar, xbs, xbr)
    ring_y = Ring(y, lambda t: at(x, t, z, core), py, rya, ryb, yas, yar, ybs, ybr)

    def ag(s, side, half):
        cols = (low, high)[half]
        dev = at(x, m4(y + (1, -1)[side]), z, core)
        return remote(
            xs.at[s, y, :, cols], xs.at[s, y, :, cols],
            ags.at[s, side, half], agr.at[s, side, half], dev,
        )

    def ag_got(s, side, half):
        cols = (low, high)[half]
        b = m4(y - (1, -1)[side])
        return remote(
            xs.at[s, b, :, cols], xs.at[s, b, :, cols],
            ags.at[s, side, half], agr.at[s, side, half], at(x, b, z, core),
        )

    def af(s, side):
        cols = (low, high)[side]
        b = m4(y - (1, -1)[side])
        dev = at(x, m4(y + (1, -1)[side]), z, core)
        return remote(
            xs.at[s, b, :, cols], xs.at[s, b, :, cols], afs.at[s, side], afr.at[s, side], dev
        )

    def af_got(s, side):
        cols = (low, high)[side]
        b = m4(y + 2)
        return remote(
            xs.at[s, b, :, cols], xs.at[s, b, :, cols], afs.at[s, side], afr.at[s, side],
            at(x, m4(y - (1, -1)[side]), z, core),
        )

    def oa(s, d):
        t = m4(x + d)
        cols = pl.ds(pl.multiple_of(t * 512, 512), 512)
        return remote(
            fin.at[s, :, cols], outb.at[x, s], oas.at[s, t], oar.at[s, x], at(t, y, z, core)
        )

    def oa_got(s, d):
        t = m4(x + d)
        cols = pl.ds(pl.multiple_of(x * 512, 512), 512)
        return remote(
            fin.at[s, :, cols], outb.at[t, s], oas.at[s, t], oar.at[s, t], at(t, y, z, core)
        )

    def od(s, t):
        return pltpu.make_async_copy(
            outb.at[t, s], out.at[pl.ds(pl.multiple_of((t * S + s) * R, R), R)], ods.at[t, s]
        )

    def project(s):
        blocks = []
        for t in range(4):
            rows = pl.ds(pl.multiple_of((t * S + s) * R, R), R)
            sides = []
            for ks, vs in ((slice(0, KA), slice(0, 512)), (slice(KA, KK), slice(512, 1024))):
                a = att[rows, vs] + dot_nt(qo[rows, ks], m_in[:, ks])
                norm = lax.rsqrt(jnp.mean(jnp.square(a), axis=1, keepdims=True) + EPS)
                u = g_s[rows, vs].astype(F32)
                a = a * norm * gain[...] * (u / (1.0 + jnp.exp(-u)))
                sides.append(a.astype(BF16))
            blocks.append(jnp.concatenate(sides, axis=1))
        gated = jnp.concatenate(blocks, axis=0)
        for n in range(4):
            cols = slice(512 * n, 512 * n + 512)
            r = dot(gated, o_s[:, cols]).astype(BF16)
            px[s, :, :, cols] = r.reshape(4, R, 512)

    def normalize(s):
        mixed = ring_x.end(s)
        rows = pl.ds(pl.multiple_of(s * R, R), R)
        stream = (res_s[rows, :].astype(F32) + mixed).astype(BF16)
        st[s] = stream
        f = stream.astype(F32)
        norm = lax.rsqrt(jnp.mean(jnp.square(f), axis=1, keepdims=True) + EPS)
        xs[s, y] = (f * norm * mgain[...]).astype(BF16)
        for half in (0, 1):
            for side in (0, 1):
                ag(s, side, half if side == 0 else 1 - half).start()

    def mix(s):
        rows = xs[s].reshape(4 * R, D)
        for n in range(2):
            cols = slice(512 * n, 512 * n + 512)
            h = jnp.maximum(dot(rows, up[:, cols]), 0.0)
            hid[:, cols] = (h * h).astype(BF16)
        for n in range(4):
            cols = slice(512 * n, 512 * n + 512)
            r = dot_nt(hid[...], down[cols, :]).astype(BF16)
            py[s, :, :, cols] = r.reshape(4, R, 512)

    def tick(tau, _):
        def stage(k, f):
            @pl.when((tau >= k) & (tau < k + S))
            def _():
                f(tau - k)

        def a_stage(s):
            project(s)
            ring_x.begin(s)

        def d_stage(s):
            for side in (0, 1):
                ag_got(s, side, side).wait_recv()
                af(s, side).start()

        def e_stage(s):
            @pl.when(s == 0)
            def _():
                for zz in range(4):
                    for p in range(4):
                        for kind in (0, 1):
                            w4_got(zz, p, kind).wait_recv()

            for side in (0, 1):
                ag_got(s, side, 1 - side).wait_recv()
                af_got(s, side).wait_recv()
            mix(s)
            ring_y.begin(s)

        def g_stage(s):
            fin[s] = (ring_y.end(s) + st[s].astype(F32)).astype(BF16)
            for d in (1, 3, 2):
                oa(s, d).start()
            outb[x, s] = fin[s, :, pl.ds(pl.multiple_of(x * 512, 512), 512)]
            od(s, x).start()

        def h_stage(s):
            for d in (1, 2, 3):
                oa_got(s, d).wait_recv()
                od(s, m4(x + d)).start()

        stage(0, a_stage)
        stage(0, near_pieces)
        stage(1, ring_x.middle)
        stage(1, far_pieces)
        stage(2, normalize)
        stage(3, d_stage)
        stage(4, e_stage)
        stage(5, ring_y.middle)
        stage(6, g_stage)
        stage(7, h_stage)
        return 0

    for d in range(4):
        own_pieces(d)
    lax.fori_loop(0, S + 7, tick, 0)

    for d in (1, 2, 3):
        w1(d).wait_send()
        for c in w2(d) + s2(d):
            c.wait_send()
    for d in range(1, 8):
        for c in s1(d) + (s3c(d),):
            c.wait_send()

    def drain(s, _):
        for kind in (0, 1):
            for side in (0, 1):
                w3(s, kind, side).wait_send()
            w3f(s, kind).wait_send()
            for zz in range(4):
                w4(zz, s, kind).wait_send()
        ring_x.drain(s)
        ring_y.drain(s)
        for side in (0, 1):
            for half in (0, 1):
                ag(s, side, half).wait_send()
            af(s, side).wait_send()
        for d in (1, 2, 3):
            oa(s, d).wait_send()
        for t in range(4):
            od(s, t).wait()
        return 0

    lax.fori_loop(0, S, drain, 0)


def body(
    residual, query_wide, key_wide, value_wide, decay_wide, gate_wide, query_narrow, key_narrow,
    value_narrow, decay_narrow, gate_narrow, head_gain, out_wide, out_narrow, mlp_gain,
    up_weight, down_weight,
):
    def v(*shape, dtype=BF16):
        return pltpu.VMEM(shape, dtype)

    def sem(*shape):
        return pltpu.SemaphoreType.DMA(shape)

    any_space = pl.BlockSpec(memory_space=pl.ANY)
    vmem = pl.BlockSpec(memory_space=pltpu.VMEM)
    scratch = [
        v(1024, KK), v(1024, KK), v(1024, KK), v(1024, 1024), v(1024, 1024), v(1024, D), v(S * R, D),
        v(4, 128, H), v(D, H), v(D, H), v(1024, KK), v(1024, KK), v(CH, 512, KK),
        v(512, KK, dtype=F32), v(512, KK), v(8, KK, dtype=F32),
        v(8, 64, KK), v(8, 8, KK, dtype=F32), v(64, KK), v(8, KK, dtype=F32),
        v(4, 64, KK), v(4, 8, KK, dtype=F32), v(8, 64, KK), v(512, KK), v(1024, 1024, dtype=F32),
        v(S, 4, R, D), v(S, 2, R, H), v(S, 2, R, D), v(S, R, D), v(S, 4, R, D),
        v(S, 4, R, D), v(S, 2, R, H), v(S, 2, R, D), v(4 * R, H), v(S, R, D), v(4, S, R, 512),
        sem(15), sem(4), sem(4), sem(2, 4), sem(2, 4), sem(2, 2, 4), sem(2, 2, 4),
        sem(2, 4), sem(2, 4), sem(2, 4, 4), sem(2, 4, 4),
        sem(8), sem(8), sem(8), sem(8), sem(4), sem(4), sem(4), sem(4), sem(8), sem(8),
        sem(S, 2), sem(S, 2), sem(S, 2, 2), sem(S, 2, 2),
        sem(S, 2), sem(S, 2), sem(S, 2, 2), sem(S, 2, 2),
        sem(S, 2, 2), sem(S, 2, 2), sem(S, 2), sem(S, 2), sem(S, 4), sem(S, 4), sem(4, S),
    ]
    return pl.pallas_call(
        kernel,
        out_shape=jax.ShapeDtypeStruct((1024, 512), BF16),
        in_specs=[any_space] * 15 + [vmem] * 2,
        out_specs=any_space,
        scratch_shapes=scratch,
        compiler_params=pltpu.CompilerParams(
            collective_id=0, has_side_effects=True, vmem_limit_bytes=67_000_000
        ),
    )(
        residual, query_wide, key_wide, value_wide, decay_wide, gate_wide, query_narrow, key_narrow,
        value_narrow, decay_narrow, gate_narrow, out_wide, out_narrow, up_weight, down_weight.T,
        head_gain.reshape(1, -1), mlp_gain.reshape(1, -1),
    )


def solution(mesh):
    return jax.shard_map(
        body,
        mesh=mesh,
        in_specs=(
            P("sp", None),
            *[P("sp", "tp")] * 10,
            P(),
            P("tp", None),
            P("tp", None),
            P(),
            P("sp", "tp"),
            P("tp", "sp"),
        ),
        out_specs=P("sp", "tp"),
        check_vma=False,
    )
```

```python
import jax
import jax.numpy as jnp
from jax import lax
from jax.experimental import pallas as pl
from jax.experimental.pallas import tpu as pltpu
from jax.sharding import PartitionSpec as P

MESH = pl.DeviceIdType.MESH
F32, BF16 = jnp.float32, jnp.bfloat16
EPS = 1e-05
C = 128
CH = 8
KA, KB, KK = 256, 128, 384
S = 8
R = 256 // S
SX = S - S // 4
BO, CO, DO, EO, FO, GO, HO = 2, 4, 5, 9, 11, 13, 15
W_TICKS = ((0, None, 1, 4), (1, None, 3, 5), (3, None, 4, 6), (2, 5, 7, 8))
D = 2048
H = 1024


def dot(a, b):
    return jnp.dot(a, b, preferred_element_type=F32)


def dot_nt(a, b):
    return lax.dot_general(a, b, (((1,), (1,)), ((), ())), preferred_element_type=F32)


def dot_tn(a, b):
    return lax.dot_general(a, b, (((0,), (0,)), ((), ())), preferred_element_type=F32)


def kernel(
    res, qw, kw, vw, dw, gw, qn, kn, vn, dn, gn, ow, on, upw, dnw, gain, mgain,
    out,
    q_s, k_s, d_s, v_s, g_s, o_s, res_s, xw, xw2, up, down, wi, offs, qo, mc, m_s, sb, dt,
    r1, rd1, t2, dt2, r2, rd2, s3, m_in, att, px, rxa, rxb, st, xs, py, rya, ryb, hid, fin, outb,
    ld, w1s, w1r, w2s, w2r, w3s, w3r, w3fr, w4s, w4r, ss, sr,
    xs_s, xar, xbr, ys_s, yar, ybr, ags, agr, afr, oas, oar, ods,
):
    sp = lax.axis_index("sp")
    x = lax.axis_index("tp")
    core = lax.rem(sp, 2)
    y = lax.rem(lax.div(sp, 2), 4)
    z = lax.div(sp, 8)
    me = lax.rem(sp, 8)

    def at(xx, yy, zz, cc):
        return ((zz * 4 + yy) * 2 + cc, xx)

    def m4(v):
        return lax.rem(v + 8, 4)

    def remote(src, dst, ss, rs, dev):
        return pltpu.make_async_remote_copy(
            src_ref=src, dst_ref=dst, send_sem=ss, recv_sem=rs, device_id=dev, device_id_type=MESH
        )

    def got(ref, sem):
        pltpu.make_async_copy(ref, ref, sem).wait()

    tok = pl.ds(pl.multiple_of(x * (S * R), S * R), S * R)
    loads = [
        (upw, xw.at[0:64]),
        (dnw, xw.at[64:128]),
        (dw, d_s.at[:, 0:KA]),
        (dn, d_s.at[:, KA:KK]),
        (kw, k_s.at[:, 0:KA]),
        (kn, k_s.at[:, KA:KK]),
        (vw, v_s.at[:, 0:512]),
        (vn, v_s.at[:, 512:1024]),
        (qw, q_s.at[:, 0:KA]),
        (qn, q_s.at[:, KA:KK]),
        (gw, g_s.at[:, 0:512]),
        (gn, g_s.at[:, 512:1024]),
        (ow, o_s.at[0:512]),
        (on, o_s.at[512:1024]),
        (res.at[tok], res_s),
    ]
    groups = (0, 0, 1, 1, 2, 2, 3, 3, 4, 4, 5, 5, 6, 6, 7)
    for (a, b), i in zip(loads, groups):
        pltpu.make_async_copy(a, b, ld.at[i]).start()

    barrier = pltpu.get_barrier_semaphore()
    for d in (1, 2, 3):
        pl.semaphore_signal(barrier, inc=1, device_id=at(m4(x + d), y, z, core), device_id_type=MESH)
        pl.semaphore_signal(barrier, inc=1, device_id=at(x, y, m4(z + d), core), device_id_type=MESH)
    for d in range(1, 8):
        j = lax.rem(me + d, 8)
        pl.semaphore_signal(barrier, inc=1, device_id=(z * 8 + j, x), device_id_type=MESH)
    for d in (1, 3):
        for dev in (at(m4(x - y - d), m4(y + d), z, core), at(m4(x + y), m4(y + d), z, core)):
            pl.semaphore_signal(barrier, inc=1, device_id=dev, device_id_type=MESH)

    own = pl.ds(pl.multiple_of(sp * 64, 64), 64)

    def w2(d):
        src = xw2 if d == 2 else xw
        dev = at(x if d == 2 else m4(x - y - d), m4(y + d), z, core)
        return (
            remote(src.at[0:64], up.at[own], w2s.at[min(d, 1)], w2r.at[y], dev),
            remote(src.at[64:128], down.at[own], w2s.at[min(d, 1)], w2r.at[y], dev),
        )

    w1 = remote(xw, xw2, w1s.at[0], w1r.at[0], at(m4(x - y - 2), y, z, core))

    def w2_start(d):
        for c in w2(d):
            if d:
                c.start()
            else:
                pl.when(y != 0)(c.start)

    row_i = lax.broadcasted_iota(jnp.int32, (C, C), 0)
    col_i = lax.broadcasted_iota(jnp.int32, (C, C), 1)
    causal = col_i <= row_i
    lower = causal.astype(BF16)
    lane = lax.broadcasted_iota(jnp.int32, (1, KK), 1)
    scale = jnp.where(lane < KA, KA**-0.5, KB**-0.5).astype(F32)
    got(d_s, ld.at[1])
    got(k_s, ld.at[2])
    got(v_s, ld.at[3])
    m_s[...] = jnp.zeros_like(m_s)

    def first(c, off):
        rows = pl.ds(pl.multiple_of(c * C, C), C)
        dd = d_s[rows, :].astype(F32)
        g = (jnp.minimum(dd, 0.0) - jnp.log1p(jnp.exp(-jnp.abs(dd)))) * (1.0 / 16.0)
        high = g.astype(BF16)
        low = (g - high.astype(F32)).astype(BF16)
        within = dot(lower, high) + dot(lower, low)
        last = within[C - 1 : C, :]
        wi[rows, :] = within
        offs[c] = off
        kd = (k_s[rows, :].astype(F32) * jnp.exp(last - within)).astype(BF16)
        mc[c] = m_s[...].astype(BF16)
        fade = jnp.exp(last)
        m_s[:, 0:KA] = m_s[:, 0:KA] * fade[:, 0:KA] + dot_tn(v_s[rows, 0:512], kd[:, 0:KA])
        m_s[:, KA:KK] = m_s[:, KA:KK] * fade[:, KA:KK] + dot_tn(v_s[rows, 512:1024], kd[:, KA:KK])
        return off + last

    total = lax.fori_loop(0, CH // 2, first, jnp.zeros((1, KK), F32))
    pl.semaphore_wait(barrier, 17)
    got(xw, ld.at[0])
    w2_start(0)
    pl.when(y != 2)(w1.start)

    @pl.when(y == 2)
    def _():
        xw2[...] = xw[...]

    total = lax.fori_loop(CH // 2, CH, first, total)
    sb[...] = m_s[...].astype(BF16)
    dt[...] = total

    def part(j):
        return pl.ds(pl.multiple_of(j * 64, 64), 64)

    def s1(d):
        j = lax.rem(me + d, 8)
        dev = (z * 8 + j, x)
        return (
            remote(sb.at[part(j)], r1.at[me], ss.at[0], sr.at[0], dev),
            remote(dt, rd1.at[me], ss.at[1], sr.at[1], dev),
        )

    for d in range(1, 8):
        for c in s1(d):
            c.start()
    r1[me] = sb[part(me), :]
    rd1[me] = dt[...]

    def piece(zz, p):
        return pl.ds(pl.multiple_of(((zz * 4 + p) * 2 + core) * 64, 64), 64)

    def w3(p, kind, side):
        ref = (up, down)[kind]
        rows = piece(z, p)
        dev = at(x, y, m4(z + (1, -1)[side]), core)
        return remote(ref.at[rows], ref.at[rows], w3s.at[0], w3r.at[p], dev)

    def w3f(p, side):
        ref = (up, down)[side]
        rows = piece(m4(z - (1, -1)[side]), p)
        dev = at(x, y, m4(z + (1, -1)[side]), core)
        return remote(ref.at[rows], ref.at[rows], w3s.at[0], w3fr.at[p], dev)

    def w4(zz, p, kind):
        ref = (up, down)[kind]
        rows = piece(zz, p)
        dev = at(x, y, z, 1 - core)
        return remote(ref.at[rows], ref.at[rows], w4s.at[0], w4r.at[0], dev)

    def own_piece(d):
        p = m4(y + d)
        if d:
            got(up.at[0:128], w2r.at[p])
        else:

            @pl.when(y != 0)
            def _():
                got(up.at[0:128], w2r.at[p])

            @pl.when(y == 0)
            def _():
                up[own, :] = xw[0:64]
                down[own, :] = xw[64:128]

        for kind, side in ((0, 0), (1, 1), (1, 0), (0, 1)):
            w3(p, kind, side).start()
        for kind in (0, 1):
            w4(z, p, kind).start()

    def near_pieces(d):
        p = m4(y + d)
        got(up.at[0:256], w3r.at[p])
        for kind in (0, 1):
            w3f(p, kind).start()
        for kind in (0, 1):
            w4(m4(z + 1), p, kind).start()
            w4(m4(z - 1), p, kind).start()

    def far_pieces(d):
        p = m4(y + d)
        got(up.at[0:128], w3fr.at[p])
        for kind in (0, 1):
            w4(m4(z + 2), p, kind).start()

    def second(c, _):
        rows = pl.ds(pl.multiple_of(c * C, C), C)
        within = wi[rows, :]
        rel = within - within[C // 2 - 1 : C // 2, :]
        qf = q_s[rows, :].astype(F32) * scale
        decayed = qf * jnp.exp(within)
        qt = (qf * jnp.exp(rel)).astype(BF16)
        kt = (k_s[rows, :].astype(F32) * jnp.exp(-rel)).astype(BF16)
        qdec = decayed.astype(BF16)
        qo[rows, :] = (decayed * jnp.exp(offs[c])).astype(BF16)
        for ks, vs in ((slice(0, KA), slice(0, 512)), (slice(KA, KK), slice(512, 1024))):
            sc = dot_nt(qt[:, ks], kt[:, ks])
            sc = jnp.where(causal, sc, 0.0).astype(BF16)
            att[rows, vs] = dot(sc, v_s[rows, vs]) + dot_nt(qdec[:, ks], mc[c, :, ks])
        return 0

    got(q_s, ld.at[4])
    lax.fori_loop(0, CH, second, 0)

    got(r1.at[0:7], sr.at[0])
    got(rd1.at[0:7], sr.at[1])

    def over_cores(j, carry):
        acc, dacc = carry
        dj = rd1[j]
        return acc * jnp.exp(dj) + r1[j].astype(F32), dacc + dj

    acc, dacc = lax.fori_loop(
        0, 8, over_cores, (jnp.zeros((64, KK), F32), jnp.zeros((1, KK), F32))
    )
    t2[...] = acc.astype(BF16)
    dt2[...] = dacc

    def s2(d):
        t = m4(z + d)
        dev = at(x, y, t, core)
        return (
            remote(t2, r2.at[z], ss.at[2], sr.at[2], dev),
            remote(dt2, rd2.at[z], ss.at[3], sr.at[3], dev),
        )

    for d in (1, 3, 2):
        for c in s2(d):
            c.start()
    r2[z] = t2[...]
    rd2[z] = dt2[...]
    w2_start(1)
    w2_start(3)
    own_piece(0)
    got(r2.at[0:3], sr.at[2])
    got(rd2.at[0:3], sr.at[3])

    def over_z(t, acc):
        return jnp.where(t < z, acc * jnp.exp(rd2[t]) + r2[t].astype(F32), acc)

    acc = lax.fori_loop(0, 4, over_z, jnp.zeros((64, KK), F32))

    def hand_out(j, acc):
        s3[j] = acc.astype(BF16)
        return acc * jnp.exp(rd1[j]) + r1[j].astype(F32)

    lax.fori_loop(0, 8, hand_out, acc)

    def s3c(d):
        j = lax.rem(me + d, 8)
        return remote(s3.at[j], m_in.at[part(me)], ss.at[4], sr.at[4], (z * 8 + j, x))

    for d in range(1, 8):
        s3c(d).start()
    m_in[part(me), :] = s3[me]
    own_piece(1)
    own_piece(3)

    got(m_in.at[0:448], sr.at[4])

    pl.when(y != 2)(w1.wait_recv)
    w2_start(2)
    got(g_s, ld.at[5])
    got(o_s, ld.at[6])
    got(res_s, ld.at[7])

    low, high = slice(0, H), slice(H, D)

    class Ring:
        def __init__(self, coord, dev, p, ra, rb, sends, a_r, b_r):
            self.c, self.dev, self.p, self.ra, self.rb = coord, dev, p, ra, rb
            self.sends, self.a_r, self.b_r = sends, a_r, b_r

        def up_of(self, s, k):
            return m4(self.c(s) + k)

        def relay(self, s, side):
            far = self.p.at[s, self.up_of(s, 2), :, (high, low)[side]]
            dev = self.dev(s, self.up_of(s, (1, -1)[side]))
            return remote(far, self.ra.at[s, side], self.sends.at[0], self.a_r.at[s], dev)

        def near(self, s, side, half):
            t = self.up_of(s, (1, -1)[side])
            cols = (low, high)[half]
            return remote(
                self.p.at[s, t, :, cols], self.rb.at[s, side, :, cols],
                self.sends.at[0], self.b_r.at[s], self.dev(s, t),
            )

        def begin(self, s):
            for side in (0, 1):
                self.relay(s, side).start()
            for side in (0, 1):
                self.near(s, side, side).start()

        def middle(self, s):
            got(self.ra.at[s], self.a_r.at[s])
            for side in (0, 1):
                t = self.up_of(s, (1, -1)[side])
                cols = (high, low)[side]
                self.p[s, t, :, cols] = (
                    self.p[s, t, :, cols].astype(F32) + self.ra[s, side].astype(F32)
                ).astype(BF16)
                self.near(s, side, 1 - side).start()

        def end(self, s):
            got(self.rb.at[s], self.b_r.at[s])
            return (
                self.p[s, self.c(s)].astype(F32)
                + self.rb[s, 0].astype(F32)
                + self.rb[s, 1].astype(F32)
            )

    def place(s):
        return jnp.where(s >= SX, x, y)

    def member(s, t):
        return at(jnp.where(s >= SX, t, x), jnp.where(s >= SX, y, t), z, core)

    ring_x = Ring(lambda s: x, lambda s, t: at(t, y, z, core), px, rxa, rxb, xs_s, xar, xbr)
    ring_y = Ring(place, member, py, rya, ryb, ys_s, yar, ybr)

    def ag(s, side, half):
        cols = (low, high)[half]
        a = place(s)
        return remote(
            xs.at[s, a, :, cols], xs.at[s, a, :, cols],
            ags.at[0], (agr if side == half else afr).at[s], member(s, m4(a + (1, -1)[side])),
        )

    def af(s, side):
        cols = (low, high)[side]
        b = m4(place(s) - (1, -1)[side])
        return remote(
            xs.at[s, b, :, cols], xs.at[s, b, :, cols],
            ags.at[0], afr.at[s], member(s, m4(place(s) + (1, -1)[side])),
        )

    def oa(s, d):
        t = m4(x + d)
        cols = pl.ds(pl.multiple_of(t * 512, 512), 512)
        return remote(
            fin.at[s, :, cols], outb.at[x, s], oas.at[0], oar.at[s], at(t, y, z, core)
        )

    def od(s, t):
        return pltpu.make_async_copy(
            outb.at[t, s], out.at[pl.ds(pl.multiple_of((t * S + s) * R, R), R)], ods.at[0]
        )

    def project(s):
        blocks = []
        for t in range(4):
            rows = pl.ds(pl.multiple_of((t * S + s) * R, R), R)
            sides = []
            for ks, vs in ((slice(0, KA), slice(0, 512)), (slice(KA, KK), slice(512, 1024))):
                a = att[rows, vs] + dot_nt(qo[rows, ks], m_in[:, ks])
                norm = lax.rsqrt(jnp.mean(jnp.square(a), axis=1, keepdims=True) + EPS)
                u = g_s[rows, vs].astype(F32)
                a = a * norm * gain[...] * (u / (1.0 + jnp.exp(-u)))
                sides.append(a.astype(BF16))
            blocks.append(jnp.concatenate(sides, axis=1))
        gated = jnp.concatenate(blocks, axis=0)
        for n in range(4):
            cols = slice(512 * n, 512 * n + 512)
            r = dot(gated, o_s[:, cols]).astype(BF16)
            px[s, :, :, cols] = r.reshape(4, R, 512)

    def normalize(s):
        mixed = ring_x.end(s)
        rows = pl.ds(pl.multiple_of(s * R, R), R)
        stream = (res_s[rows, :].astype(F32) + mixed).astype(BF16)
        st[s] = stream
        f = stream.astype(F32)
        norm = lax.rsqrt(jnp.mean(jnp.square(f), axis=1, keepdims=True) + EPS)
        xs[s, place(s)] = (f * norm * mgain[...]).astype(BF16)
        for half in (0, 1):
            for side in (0, 1):
                ag(s, side, half if side == 0 else 1 - half).start()

    def mix(s):
        rows = xs[s].reshape(4 * R, D)
        for n in range(2):
            cols = slice(512 * n, 512 * n + 512)
            h = jnp.maximum(dot(rows, up[:, cols]), 0.0)
            hid[:, cols] = (h * h).astype(BF16)
        for n in range(4):
            cols = slice(512 * n, 512 * n + 512)
            r = dot_nt(hid[...], down[cols, :]).astype(BF16)
            py[s, :, :, cols] = r.reshape(4, R, 512)

    def tick(tau, _):
        def stage(k, f):
            @pl.when((tau >= k) & (tau < k + S))
            def _():
                f(tau - k)

        def once(k, f, d):
            @pl.when(tau == k)
            def _():
                f(d)

        def a_stage(s):
            project(s)
            ring_x.begin(s)

        def d_stage(s):
            got(rya.at[s], agr.at[s])
            for side in (0, 1):
                af(s, side).start()

        def e_stage(s):
            @pl.when(s == 0)
            def _():
                got(up, w4r.at[0])

            got(ryb.at[s], afr.at[s])
            mix(s)
            ring_y.begin(s)

        def g_stage(s):
            fin[s] = (ring_y.end(s) + st[s].astype(F32)).astype(BF16)
            for d in (1, 3, 2):
                oa(s, d).start()
            outb[x, s] = fin[s, :, pl.ds(pl.multiple_of(x * 512, 512), 512)]
            od(s, x).start()

        def h_stage(s):
            got(outb.at[0:3, s], oar.at[s])
            for d in (1, 2, 3):
                od(s, m4(x + d)).start()

        stage(0, a_stage)
        for d, mine, near, far in W_TICKS:
            if mine is not None:
                once(mine, own_piece, d)
        for d, mine, near, far in W_TICKS:
            once(near, near_pieces, d)
        for d, mine, near, far in W_TICKS:
            once(far, far_pieces, d)
        stage(BO, ring_x.middle)
        stage(CO, normalize)
        stage(DO, d_stage)
        stage(EO, e_stage)
        stage(FO, ring_y.middle)
        stage(GO, g_stage)
        stage(HO, h_stage)
        return 0

    lax.fori_loop(0, S + HO, tick, 0)

    @pl.when(y != 0)
    def _():
        got(up.at[0:128], w2s.at[0])

    pl.when(y != 2)(w1.wait_send)
    got(up.at[0:384], w2s.at[1])
    got(r1.at[0:7], ss.at[0])
    got(rd1.at[0:7], ss.at[1])
    got(r2.at[0:3], ss.at[2])
    got(rd2.at[0:3], ss.at[3])
    got(m_in.at[0:448], ss.at[4])
    got(up.at[0:1536], w3s.at[0])
    got(up, w4s.at[0])
    for sends in (xs_s, ys_s, ags):
        got(up.at[0:1536], sends.at[0])
    got(outb.at[0:3], oas.at[0])
    got(outb, ods.at[0])


def body(
    residual, query_wide, key_wide, value_wide, decay_wide, gate_wide, query_narrow, key_narrow,
    value_narrow, decay_narrow, gate_narrow, head_gain, out_wide, out_narrow, mlp_gain,
    up_weight, down_weight,
):
    def v(*shape, dtype=BF16):
        return pltpu.VMEM(shape, dtype)

    def sem(*shape):
        return pltpu.SemaphoreType.DMA(shape)

    any_space = pl.BlockSpec(memory_space=pl.ANY)
    vmem = pl.BlockSpec(memory_space=pltpu.VMEM)
    scratch = [
        v(1024, KK), v(1024, KK), v(1024, KK), v(1024, 1024), v(1024, 1024), v(1024, D), v(S * R, D),
        v(128, H), v(128, H), v(D, H), v(D, H), v(1024, KK, dtype=F32), v(CH, 1, KK, dtype=F32), v(1024, KK), v(CH, 512, KK),
        v(512, KK, dtype=F32), v(512, KK), v(1, KK, dtype=F32),
        v(8, 64, KK), v(8, 1, KK, dtype=F32), v(64, KK), v(1, KK, dtype=F32),
        v(4, 64, KK), v(4, 1, KK, dtype=F32), v(8, 64, KK), v(512, KK), v(1024, 1024, dtype=F32),
        v(S, 4, R, D), v(S, 2, R, H), v(S, 2, R, D), v(S, R, D), v(S, 4, R, D),
        v(S, 4, R, D), v(S, 2, R, H), v(S, 2, R, D), v(4 * R, H), v(S, R, D), v(4, S, R, 512),
        sem(8), sem(1), sem(1), sem(2), sem(4), sem(1), sem(4), sem(4), sem(1), sem(1), sem(5), sem(5),
        sem(1), sem(S), sem(S), sem(1), sem(S), sem(S), sem(1), sem(S), sem(S), sem(1), sem(S), sem(1),
    ]
    return pl.pallas_call(
        kernel,
        out_shape=jax.ShapeDtypeStruct((1024, 512), BF16),
        in_specs=[any_space] * 15 + [vmem] * 2,
        out_specs=any_space,
        scratch_shapes=scratch,
        compiler_params=pltpu.CompilerParams(
            collective_id=0, has_side_effects=True, vmem_limit_bytes=67_000_000
        ),
    )(
        residual, query_wide, key_wide, value_wide, decay_wide, gate_wide, query_narrow, key_narrow,
        value_narrow, decay_narrow, gate_narrow, out_wide, out_narrow, up_weight, down_weight.T,
        head_gain.reshape(1, -1), mlp_gain.reshape(1, -1),
    )


def solution(mesh):
    return jax.shard_map(
        body,
        mesh=mesh,
        in_specs=(
            P("sp", None),
            *[P("sp", "tp")] * 10,
            P(),
            P("tp", None),
            P("tp", None),
            P(),
            P("sp", "tp"),
            P("tp", "sp"),
        ),
        out_specs=P("sp", "tp"),
        check_vma=False,
    )
```
